32 devices in a mesh: rep: 2 (over x), fs: 8 (over z, y), tp: 2 (over core).
Axes of the slice: x: 2, y: 2, z: 4, core: 2. Of those that a mesh axis runs over, the one named last changes fastest.
Arguments:
- tokens: bfloat16 [16, 64, 2048], P(('rep', 'fs'), None, 'tp'), may hold values from -6 to 6
- lin_weight: bfloat16 [2048, 1024], P('fs', 'tp'), may hold values from -0.125 to 0.125
- glu_weight: bfloat16 [2048, 1024], P('fs', 'tp'), may hold values from -0.125 to 0.125
- conv_taps: float32 [31, 1024], P(None, 'tp'), may hold values from -4 to 4
- conv_gain: float32 [1024], P('tp'), may hold values from 0.1 to 1.9
- conv_out_weight: bfloat16 [1024, 2048], P('tp', 'fs'), may hold values from -0.1875 to 0.1875
- mix_gain: float32 [2048], replicated, may hold values from 0.1 to 1.9
- ff_gate: bfloat16 [2048, 5632], P('fs', 'tp'), may hold values from -0.125 to 0.125
- ff_up: bfloat16 [2048, 5632], P('fs', 'tp'), may hold values from -0.125 to 0.125
- ff_down: bfloat16 [5632, 2048], P('tp', 'fs'), may hold values from -0.078125 to 0.078125
- out_gain: float32 [2048], replicated, may hold values from 0.1 to 1.9
Outputs:
- encoded: bfloat16 [16, 64, 2048], P(('rep', 'fs'), None, 'tp')
The draws below stay inside these ranges and needn't reach their ends.
All inputs are finite; a program needn't handle non-finite values.
Results may differ from the reference program's by a relative error of at most 0.014.
Values may be sent and summed in bfloat16 or wider, within the bound.
A program may use at most 128 MiB of HBM per device.

```python
import jax
import jax.numpy as jnp
from jax import lax

D = 2048
CONV = 1024
FF = 5632
TAPS = 31
TOK_DEV = 64
SEQUENCES = 16
N_TP = 2


def draw_conv_taps(key, part):
    first, second = jax.random.split(jax.random.fold_in(key, 17))
    channel = jnp.arange(CONV, dtype=jnp.float32)
    ramp = 3.0 ** (2.0 * channel / CONV - 1.0)
    spread = jnp.exp(jax.random.uniform(second, (CONV,), jnp.float32, -0.5, 0.5))
    base = jnp.clip(jax.random.normal(first, (TAPS, CONV), jnp.float32), -4.0, 4.0)
    return (base * TAPS ** (-0.5) * ramp * spread).astype(jnp.float32)


def shard_levels(key, shape, cuts, smallest, largest):
    def one(dim, parts):
        steps = jax.random.uniform(jax.random.fold_in(jax.random.fold_in(key, 6), dim), (parts,), jnp.float32, smallest / len(cuts), largest / len(cuts))
        return jnp.repeat(jnp.exp(steps), shape[dim] // parts).reshape((-1,) + (1,) * (len(shape) - dim - 1))

    factor_of = one(*cuts[0])
    for cut in cuts[1:]:
        factor_of = factor_of * one(*cut)
    return factor_of


def bell_draw(own_key, dims, deviation, bound, pieces=(), kind=jnp.bfloat16):
    values = deviation * jax.random.normal(own_key, dims, jnp.float32)
    if pieces:
        values = values * shard_levels(own_key, dims, pieces, -0.22, 0.18)
    return jnp.clip(values, -bound, bound).astype(kind)


def setup_inputs(seed: int = 0) -> dict:
    keys = jax.random.split(jax.random.key(seed), 12)
    return {
        "tokens": bell_draw(keys[0], (SEQUENCES, TOK_DEV, D), 1.0, 6.0, ((0, 16), (2, 2))),
        "lin_weight": bell_draw(keys[1], (D, CONV), D ** -0.5, 0.125, ((0, 8), (1, 2))),
        "glu_weight": bell_draw(keys[2], (D, CONV), D ** -0.5, 0.125, ((0, 8), (1, 2))),
        "conv_taps": draw_conv_taps(jax.random.fold_in(keys[11], 71), 0),
        "conv_gain": jnp.clip(1.0 + 0.18 * jax.random.normal(keys[4], (CONV,), jnp.float32), 0.1, 1.9),
        "conv_out_weight": bell_draw(keys[5], (CONV, D), CONV ** -0.5, 0.1875, ((0, 2), (1, 8))),
        "mix_gain": jnp.clip(1.0 + 0.18 * jax.random.normal(keys[6], (D,), jnp.float32), 0.1, 1.9),
        "ff_gate": bell_draw(keys[7], (D, FF), D ** -0.5, 0.125, ((0, 8), (1, 2))),
        "ff_up": bell_draw(keys[8], (D, FF), D ** -0.5, 0.125, ((0, 8), (1, 2))),
        "ff_down": bell_draw(keys[9], (FF, D), FF ** -0.5, 0.078125, ((0, 2), (1, 8))),
        "out_gain": jnp.clip(1.0 + 0.18 * jax.random.normal(keys[10], (D,), jnp.float32), 0.1, 1.9),
    }


residual_scale = 2.0 ** 0.25
epsilon = 1e-05

def rounded(value):
    return lax.optimization_barrier(value.astype(jnp.bfloat16)).astype(jnp.float32)

def normalize(values):
    average = lax.optimization_barrier(jnp.mean(values, axis=-1, keepdims=True))
    squares = lax.optimization_barrier(jnp.mean(values * values, axis=-1, keepdims=True))
    return (values - average) * lax.rsqrt(squares - average * average + epsilon)

def block_sum(left, right):
    rows, inner = left.shape
    width = inner // N_TP
    left_blocks = left.astype(jnp.float32).reshape(rows, N_TP, width)
    right_blocks = right.astype(jnp.float32).reshape(N_TP, width, right.shape[1])
    partial_value = jnp.einsum('tjc,jcd->jtd', left_blocks, right_blocks)
    return lax.optimization_barrier(jnp.sum(rounded(partial_value), axis=0))

def depthwise(values, conv_taps):
    margin = (TAPS - 1) // 2
    return lax.conv_general_dilated(values[None], conv_taps[:, None, :], (1,), [(margin, margin)], dimension_numbers=('NWC', 'WIO', 'NWC'), feature_group_count=values.shape[1], precision=lax.Precision.HIGHEST)[0]

def reference(tokens, lin_weight, glu_weight, conv_taps, conv_gain, conv_out_weight, mix_gain, ff_gate, ff_up, ff_down, out_gain):

    def one_sequence(inputs):
        linear = jnp.dot(inputs, lin_weight, preferred_element_type=jnp.float32)
        gating = jnp.dot(inputs, glu_weight, preferred_element_type=jnp.float32)
        glu = (linear * jax.nn.sigmoid(gating)).astype(jnp.bfloat16)
        conv = depthwise(glu.astype(jnp.float32), conv_taps)
        activated = jax.nn.silu(normalize(conv) * conv_gain).astype(jnp.bfloat16)
        mixed = rounded(block_sum(activated, conv_out_weight))
        middle = (normalize(residual_scale * inputs.astype(jnp.float32) + mixed) * mix_gain).astype(jnp.bfloat16)
        gate = jnp.dot(middle, ff_gate, preferred_element_type=jnp.float32)
        upward = jnp.dot(middle, ff_up, preferred_element_type=jnp.float32)
        hidden = (jax.nn.silu(gate) * upward).astype(jnp.bfloat16)
        forward = rounded(block_sum(hidden, ff_down))
        total = residual_scale * middle.astype(jnp.float32) + forward
        return (normalize(total) * out_gain).astype(jnp.bfloat16)
    return lax.map(one_sequence, tokens)
```

```python
import jax
import jax.numpy as jnp
from jax import lax
from jax.sharding import PartitionSpec as P

residual_scale = 2.0**0.25
epsilon = 1e-05


def normed(values):
    average = jnp.mean(values, axis=-1, keepdims=True)
    second = jnp.mean(values * values, axis=-1, keepdims=True)
    return (values - average) * lax.rsqrt(second - average * average + epsilon)


def interleave(left, right, parts):
    rows, width = left.shape
    pair = jnp.concatenate(
        (left.reshape(rows, parts, width // parts), right.reshape(rows, parts, width // parts)),
        axis=2,
    )
    return pair.reshape(rows, 2 * width)


def on_device(
    tokens,
    lin_weight,
    glu_weight,
    conv_taps,
    conv_gain_all,
    conv_out_weight,
    mix_gain,
    ff_gate,
    ff_up,
    ff_down,
    out_gain,
):
    n_fs, n_tp = lax.axis_size("fs"), lax.axis_size("tp")
    fs_index, tp_index = lax.axis_index("fs"), lax.axis_index("tp")
    seqs, length, feat = tokens.shape
    groups = n_fs * seqs
    rows = groups * length
    model = feat * n_tp

    gathered = lax.all_gather(tokens, ("fs", "tp"), axis=0, tiled=False)
    all_tokens = (
        gathered.reshape(n_fs, n_tp, seqs, length, feat)
        .transpose(0, 2, 3, 1, 4)
        .reshape(rows, model)
    )
    glu_pair = lax.all_to_all(
        interleave(lin_weight, glu_weight, n_fs), "fs", split_axis=1, concat_axis=0, tiled=True
    )
    own_out = lax.all_to_all(conv_out_weight, "tp", split_axis=1, concat_axis=0, tiled=True)
    ff_pair = lax.all_to_all(
        interleave(ff_gate, ff_up, n_fs), "fs", split_axis=1, concat_axis=0, tiled=True
    )
    own_down = lax.all_to_all(ff_down, "fs", split_axis=0, concat_axis=1, tiled=True)

    chans = glu_pair.shape[1] // 2
    product = jnp.dot(all_tokens, glu_pair, preferred_element_type=jnp.float32)
    glu = (product[:, :chans] * jax.nn.sigmoid(product[:, chans:])).astype(jnp.bfloat16)
    n_taps = conv_taps.shape[0]
    margin = (n_taps - 1) // 2
    own_taps = lax.dynamic_slice_in_dim(conv_taps, fs_index * chans, chans, 1)
    padded = jnp.pad(
        glu.astype(jnp.float32).reshape(groups, length, chans),
        ((0, 0), (margin, margin), (0, 0)),
    )
    conv = sum(padded[:, k : k + length] * own_taps[k] for k in range(n_taps))
    conv = conv.reshape(rows, chans).astype(jnp.bfloat16)
    conv_all = lax.all_gather(conv, ("tp", "fs"), axis=1, tiled=True)
    activated = jax.nn.silu(normed(conv_all.astype(jnp.float32)) * conv_gain_all).astype(
        jnp.bfloat16
    )
    mixed_own = jnp.dot(activated, own_out, preferred_element_type=jnp.float32).astype(
        jnp.bfloat16
    )
    mixed = lax.all_gather(mixed_own, ("fs", "tp"), axis=1, tiled=True)
    before = residual_scale * all_tokens.astype(jnp.float32) + mixed.astype(jnp.float32)
    middle = (normed(before) * mix_gain).astype(jnp.bfloat16)

    units = ff_pair.shape[1] // 2
    both = jnp.dot(middle, ff_pair, preferred_element_type=jnp.float32)
    hidden = (jax.nn.silu(both[:, :units]) * both[:, units:]).astype(jnp.bfloat16)
    down = jnp.dot(hidden, own_down, preferred_element_type=jnp.float32).astype(jnp.bfloat16)
    sends = (
        down.reshape(n_fs, seqs * length, n_tp, feat)
        .transpose(0, 2, 1, 3)
        .reshape(n_fs * n_tp, seqs * length, feat)
    )
    arrived = lax.all_to_all(sends, ("fs", "tp"), split_axis=0, concat_axis=0, tiled=True)
    forward = jnp.sum(arrived.astype(jnp.float32), axis=0)
    forward = forward.astype(jnp.bfloat16).astype(jnp.float32)
    middle_own = lax.dynamic_slice(
        middle,
        (fs_index * seqs * length, tp_index * feat),
        (seqs * length, feat),
    )
    final = residual_scale * middle_own.astype(jnp.float32) + forward
    sums, squares = lax.psum(
        (jnp.sum(final, axis=1, keepdims=True), jnp.sum(final * final, axis=1, keepdims=True)),
        "tp",
    )
    average = sums / model
    out = (final - average) * lax.rsqrt(squares / model - average * average + epsilon)
    gain = lax.dynamic_slice_in_dim(out_gain, tp_index * feat, feat, 0)
    return (out * gain).astype(jnp.bfloat16).reshape(seqs, length, feat)


def solution(mesh):
    mapped = jax.shard_map(
        on_device,
        mesh=mesh,
        in_specs=(
            P(("rep", "fs"), None, "tp"),
            P("fs", "tp"),
            P("fs", "tp"),
            P(None, "tp"),
            P(),
            P("tp", "fs"),
            P(),
            P("fs", "tp"),
            P("fs", "tp"),
            P("tp", "fs"),
            P(),
        ),
        out_specs=P(("rep", "fs"), None, "tp"),
        check_vma=False,
    )
    return mapped
```

```python
import functools

import jax
import jax.numpy as jnp
from jax import lax
from jax.experimental import pallas as pl
from jax.experimental.pallas import tpu as pltpu
from jax.sharding import PartitionSpec as P

residual_scale = 2.0**0.25
epsilon = 1e-05


def normed(values):
    average = jnp.mean(values, axis=-1, keepdims=True)
    second = jnp.mean(values * values, axis=-1, keepdims=True)
    return (values - average) * lax.rsqrt(second - average * average + epsilon)


def interleave(left, right, parts):
    rows, width = left.shape
    pair = jnp.concatenate(
        (left.reshape(rows, parts, width // parts), right.reshape(rows, parts, width // parts)),
        axis=2,
    )
    return pair.reshape(rows, 2 * width)


def by_collectives(
    tokens,
    lin_weight,
    glu_weight,
    conv_taps,
    conv_gain,
    conv_out_weight,
    mix_gain,
    ff_gate,
    ff_up,
    ff_down,
    out_gain,
):
    n_fs, n_tp = lax.axis_size("fs"), lax.axis_size("tp")
    fs_index, tp_index = lax.axis_index("fs"), lax.axis_index("tp")
    seqs, length, feat = tokens.shape
    groups = n_fs * seqs
    rows = groups * length
    model = feat * n_tp
    conv_gain_all = lax.all_gather(conv_gain, "tp", axis=0, tiled=True)

    gathered = lax.all_gather(tokens, ("fs", "tp"), axis=0, tiled=False)
    all_tokens = (
        gathered.reshape(n_fs, n_tp, seqs, length, feat)
        .transpose(0, 2, 3, 1, 4)
        .reshape(rows, model)
    )
    glu_pair = lax.all_to_all(
        interleave(lin_weight, glu_weight, n_fs), "fs", split_axis=1, concat_axis=0, tiled=True
    )
    own_out = lax.all_to_all(conv_out_weight, "tp", split_axis=1, concat_axis=0, tiled=True)
    ff_pair = lax.all_to_all(
        interleave(ff_gate, ff_up, n_fs), "fs", split_axis=1, concat_axis=0, tiled=True
    )
    own_down = lax.all_to_all(ff_down, "fs", split_axis=0, concat_axis=1, tiled=True)

    chans = glu_pair.shape[1] // 2
    product = jnp.dot(all_tokens, glu_pair, preferred_element_type=jnp.float32)
    glu = (product[:, :chans] * jax.nn.sigmoid(product[:, chans:])).astype(jnp.bfloat16)
    n_taps = conv_taps.shape[0]
    margin = (n_taps - 1) // 2
    own_taps = lax.dynamic_slice_in_dim(conv_taps, fs_index * chans, chans, 1)
    padded = jnp.pad(
        glu.astype(jnp.float32).reshape(groups, length, chans),
        ((0, 0), (margin, margin), (0, 0)),
    )
    conv = sum(padded[:, k : k + length] * own_taps[k] for k in range(n_taps))
    conv = conv.reshape(rows, chans).astype(jnp.bfloat16)
    conv_all = lax.all_gather(conv, ("tp", "fs"), axis=1, tiled=True)
    activated = jax.nn.silu(normed(conv_all.astype(jnp.float32)) * conv_gain_all).astype(
        jnp.bfloat16
    )
    mixed_own = jnp.dot(activated, own_out, preferred_element_type=jnp.float32).astype(
        jnp.bfloat16
    )
    mixed = lax.all_gather(mixed_own, ("fs", "tp"), axis=1, tiled=True)
    before = residual_scale * all_tokens.astype(jnp.float32) + mixed.astype(jnp.float32)
    middle = (normed(before) * mix_gain).astype(jnp.bfloat16)

    units = ff_pair.shape[1] // 2
    both = jnp.dot(middle, ff_pair, preferred_element_type=jnp.float32)
    hidden = (jax.nn.silu(both[:, :units]) * both[:, units:]).astype(jnp.bfloat16)
    down = jnp.dot(hidden, own_down, preferred_element_type=jnp.float32).astype(jnp.bfloat16)
    sends = (
        down.reshape(n_fs, seqs * length, n_tp, feat)
        .transpose(0, 2, 1, 3)
        .reshape(n_fs * n_tp, seqs * length, feat)
    )
    arrived = lax.all_to_all(sends, ("fs", "tp"), split_axis=0, concat_axis=0, tiled=True)
    forward = jnp.sum(arrived.astype(jnp.float32), axis=0)
    forward = forward.astype(jnp.bfloat16).astype(jnp.float32)
    middle_own = lax.dynamic_slice(
        middle,
        (fs_index * seqs * length, tp_index * feat),
        (seqs * length, feat),
    )
    final = residual_scale * middle_own.astype(jnp.float32) + forward
    sums, squares = lax.psum(
        (jnp.sum(final, axis=1, keepdims=True), jnp.sum(final * final, axis=1, keepdims=True)),
        "tp",
    )
    average = sums / model
    out = (final - average) * lax.rsqrt(squares / model - average * average + epsilon)
    gain = lax.dynamic_slice_in_dim(out_gain, tp_index * feat, feat, 0)
    return (out * gain).astype(jnp.bfloat16).reshape(seqs, length, feat)


MESH = pl.DeviceIdType.MESH
LANES = 128


def fused(
    n_fs,
    n_tp,
    width,
    tok,
    glu_mix,
    taps,
    gain,
    out_weight,
    mix_gain,
    gate_hbm,
    up_hbm,
    down_hbm,
    out_gain,
    out,
    x_s,
    glu_s,
    gain_s,
    proj_s,
    pad_s,
    conv_s,
    norm_s,
    act_s,
    mixed_s,
    mid_s,
    gate_s,
    up_s,
    down_s,
    hid_s,
    part_s,
    half_s,
    sum_s,
    q_s,
    stat_s,
    glu_sems,
    small_sems,
    tok_sems,
    conv_sems,
    mixed_sems,
    ff_sems,
    cross_sems,
    local_sems,
    half_sems,
    q_sems,
):
    rep, f, t = lax.axis_index("rep"), lax.axis_index("fs"), lax.axis_index("tp")
    other = 1 - t
    n_hi = n_fs // 2
    hi, lo = f // 2, f % 2
    rows, feat = x_s.shape[1:]
    length = rows // n_fs
    model = feat * n_tp
    depth = gate_hbm.shape[0]
    half_depth = depth // 2
    total = gate_hbm.shape[1]
    chans = LANES // 2
    pending = []

    barrier = pltpu.get_barrier_semaphore()
    for d in range(n_fs):
        for e in range(n_tp):
            if d or e:
                pl.semaphore_signal(
                    barrier,
                    inc=1,
                    device_id=(rep, (f + d) % n_fs, (t + e) % n_tp),
                    device_id_type=MESH,
                )
    pl.semaphore_signal(barrier, inc=1, device_id=(1 - rep, f, t), device_id_type=MESH)
    pl.semaphore_wait(barrier, n_fs * n_tp)

    def remote(src, dst, sems, index, device):
        return pltpu.make_async_remote_copy(
            src_ref=src,
            dst_ref=dst,
            send_sem=sems.at[0, index],
            recv_sem=sems.at[1, index],
            device_id=device,
            device_id_type=MESH,
        )

    def send(*parts):
        copy = remote(*parts)
        copy.start()
        pending.append(copy)

    partner = (rep, f, other)

    def receive(dst, sems, index):
        remote(dst, dst, sems, index, partner).wait_recv()

    def at(step, low):
        return ((hi - step + n_hi) % n_hi) * 2 + low

    def gather_start(own, slot, sems):
        for d in range(1, n_hi):
            send(own, slot(f, t), sems, d, (rep, ((hi + d) % n_hi) * 2 + lo, t))
        send(own, slot(f, t), sems, n_hi, (rep, hi * 2 + 1 - lo, t))
        send(own, slot(f, t), sems, 2 * n_hi, partner)

    def gather_finish(slot, sems):
        for d in range(1, n_hi):
            block = slot(at(d, lo), t)
            receive(block, sems, d)
            send(block, block, sems, n_hi + d, (rep, hi * 2 + 1 - lo, t))
            send(block, block, sems, 2 * n_hi + d, partner)
        for d in range(n_hi):
            block = slot(at(d, 1 - lo), t)
            receive(block, sems, n_hi + d)
            send(block, block, sems, 3 * n_hi + d, partner)
        for d in range(n_hi):
            receive(slot(at(d, lo), other), sems, 2 * n_hi + d)
            receive(slot(at(d, 1 - lo), other), sems, 3 * n_hi + d)

    def tok_slot(i, j):
        return x_s.at[j, pl.ds(pl.multiple_of(i * length, length), length)]

    def glu_slot(i):
        return glu_s.at[pl.ds(pl.multiple_of(i * depth, depth), depth)]

    gather_start(tok, tok_slot, tok_sems)
    for d in range(1, n_fs):
        to = (f + d) % n_fs
        send(glu_mix.at[to], glu_slot(f), glu_sems, d, (rep, to, t))
    send(gain, gain_s.at[t], small_sems, 0, partner)
    columns = pl.ds(pl.multiple_of(other * LANES, LANES), LANES)
    own_columns = pl.ds(pl.multiple_of(t * LANES, LANES), LANES)
    send(out_weight.at[:, columns], proj_s.at[t], small_sems, 1, partner)

    def start_of(i):
        return pl.multiple_of(i * width - (i // (n_fs - 1)) * (n_fs * width - total), LANES)

    half_width = width // 2

    def pieces(to, source, part):
        first = start_of(to)
        ups = pl.ds(pl.multiple_of(part * half_depth, half_depth), half_depth)
        spot = pl.ds(pl.multiple_of(source * depth + part * half_depth, half_depth), half_depth)
        deep = pl.ds(pl.multiple_of(part * half_width, half_width), half_width)
        from_down = pl.ds(pl.multiple_of(first + part * half_width, LANES // 2), half_width)
        return (
            (gate_hbm.at[ups, pl.ds(first, width)], gate_s.at[spot]),
            (up_hbm.at[ups, pl.ds(first, width)], up_s.at[spot]),
            (down_hbm.at[from_down], down_s.at[source, deep]),
        )

    order = range(1, n_fs)

    def weights_start(which):
        for d in order:
            to = (f + d) % n_fs
            src, dst = pieces(to, f, rep)[which]
            send(src, dst, ff_sems, which * n_fs + d, (rep, to, t))

    def weights_forward(which):
        for d in order:
            dst = pieces(f, (f - d + n_fs) % n_fs, rep)[which][1]
            receive(dst, ff_sems, which * n_fs + d)
            send(dst, dst, cross_sems, which * n_fs + d, (1 - rep, f, t))

    def weights_finish(which):
        for d in order:
            dst = pieces(f, (f - d + n_fs) % n_fs, 1 - rep)[which][1]
            receive(dst, cross_sems, which * n_fs + d)

    weights_start(0)
    weights_start(1)
    own_copies = []
    for which in range(3):
        for part in range(2):
            src, dst = pieces(f, f, part)[which]
            own_copies.append(
                pltpu.make_async_copy(src, dst, local_sems.at[which * 2 + part])
            )
    for copy in own_copies:
        copy.start()

    x_s[t, pl.ds(pl.multiple_of(f * length, length), length), :] = tok[...]
    glu_s[pl.ds(pl.multiple_of(f * depth, depth), depth), :] = glu_mix[f]
    gain_s[t] = gain[...]
    proj_s[t] = out_weight[:, own_columns]
    pad_s[...] = jnp.zeros_like(pad_s)

    gather_finish(tok_slot, tok_sems)
    for d in range(1, n_fs):
        receive(glu_slot((f - d + n_fs) % n_fs), glu_sems, d)

    product = sum(
        jnp.dot(
            x_s[j], glu_s[j * feat : (j + 1) * feat], preferred_element_type=jnp.float32
        )
        for j in range(n_tp)
    )
    glu = product[:, :chans] / (1.0 + jnp.exp(-product[:, chans:]))
    top = rows // 2
    packed = jnp.concatenate((glu[:top], glu[top:]), axis=1)
    packed = packed.astype(jnp.bfloat16).astype(jnp.float32)
    n_taps = taps.shape[0]
    margin = (n_taps - 1) // 2
    conv_slot = lambda i, j: conv_s.at[j * n_fs + i]
    groups = n_fs // 2
    for g in range(groups):
        pad_s[g, 16 : 16 + length, :] = packed[g * length : (g + 1) * length]
    for g in range(groups):
        acc = jnp.zeros((length, LANES), jnp.float32)
        for k in range(n_taps):
            first = 16 - margin + k
            acc = acc + pad_s[g, first : first + length, :] * taps[k : k + 1, :]
        conv_s[t * n_fs + f, g * length : (g + 1) * length, :] = acc.astype(jnp.bfloat16)
    gather_start(conv_slot(f, t), conv_slot, conv_sems)
    weights_forward(0)
    gather_finish(conv_slot, conv_sems)
    receive(gain_s.at[other], small_sems, 0)
    receive(proj_s.at[other], small_sems, 1)

    for j in range(n_fs * n_tp // 2):
        left = conv_s[2 * j].astype(jnp.float32)
        right = conv_s[2 * j + 1].astype(jnp.float32)
        cols = slice(j * LANES, (j + 1) * LANES)
        norm_s[:top, cols] = jnp.concatenate((left[:, :chans], right[:, :chans]), axis=1)
        norm_s[top:, cols] = jnp.concatenate((left[:, chans:], right[:, chans:]), axis=1)
    gains = jnp.concatenate([gain_s[j] for j in range(n_tp)], axis=1)

    @pl.loop(0, n_fs)
    def _(i):
        here = pl.ds(pl.multiple_of(i * length, length), length)
        v = normed(norm_s[here, :]) * gains
        act_s[here, :] = (v / (1.0 + jnp.exp(-v))).astype(jnp.bfloat16)

    share = proj_s.shape[1]
    mixed_slot = lambda i, j: mixed_s.at[i * n_tp + j]
    mixed_s[f * n_tp + t] = sum(
        jnp.dot(
            act_s[:, j * share : (j + 1) * share],
            proj_s[j],
            preferred_element_type=jnp.float32,
        )
        for j in range(n_tp)
    ).astype(jnp.bfloat16)
    gather_start(mixed_slot(f, t), mixed_slot, mixed_sems)
    weights_start(2)
    weights_forward(1)
    gather_finish(mixed_slot, mixed_sems)

    @pl.loop(0, n_fs)
    def _(i):
        here = pl.ds(pl.multiple_of(i * length, length), length)
        skip = jnp.concatenate([x_s[j, here, :] for j in range(n_tp)], axis=1)
        added = jnp.concatenate([mixed_s[j, here, :] for j in range(n_fs * n_tp)], axis=1)
        before = residual_scale * skip.astype(jnp.float32) + added.astype(jnp.float32)
        mid_s[here, :] = (normed(before) * mix_gain[...]).astype(jnp.bfloat16)

    for copy in own_copies:
        copy.wait()
    weights_finish(0)
    weights_finish(1)
    weights_forward(2)
    keep = lax.broadcasted_iota(jnp.int32, (1, width), 1) + start_of(f) >= f * width

    @pl.loop(0, 2)
    def _(i):
        here = pl.ds(pl.multiple_of(i * top, top), top)
        gate = jnp.dot(mid_s[here, :], gate_s[...], preferred_element_type=jnp.float32)
        upward = jnp.dot(mid_s[here, :], up_s[...], preferred_element_type=jnp.float32)
        value = gate / (1.0 + jnp.exp(-gate)) * upward
        hid_s[here, :] = jnp.where(keep, value, 0.0).astype(jnp.bfloat16)

    weights_finish(2)
    span = down_s.shape[2]
    per_half = n_fs // n_tp

    @pl.loop(0, n_fs)
    def _(j):
        place = pl.ds(pl.multiple_of((j % per_half) * span, span), span)
        part_s[j // per_half, :, place] = jnp.dot(
            hid_s[...], down_s[j], preferred_element_type=jnp.float32
        ).astype(jnp.bfloat16)

    def rows_of(i):
        return pl.ds(pl.multiple_of(i * length, length), length)

    for d in list(range(1, n_fs)) + [0]:
        here = rows_of((f + d) % n_fs)
        send(part_s.at[other, here], half_s.at[here], half_sems, d, partner)
    for d in list(range(1, n_fs)) + [0]:
        to = (f + d) % n_fs
        here = rows_of(to)
        receive(half_s.at[here], half_sems, d)
        both = part_s[t, here, :].astype(jnp.float32) + half_s[here, :].astype(jnp.float32)
        sum_s[here, :] = both.astype(jnp.bfloat16)
        if d:
            send(sum_s.at[here], q_s.at[f], q_sems, d, (rep, to, t))
    forward = sum_s[rows_of(f), :].astype(jnp.float32)
    for d in range(1, n_fs):
        source = (f - d + n_fs) % n_fs
        receive(q_s.at[source], q_sems, d)
        forward = forward + q_s[source].astype(jnp.float32)
    forward = forward.astype(jnp.bfloat16).astype(jnp.float32)
    own_half = pl.ds(pl.multiple_of(t * feat, feat), feat)
    final = residual_scale * mid_s[rows_of(f), own_half].astype(jnp.float32) + forward
    lane = lax.broadcasted_iota(jnp.int32, (length, LANES), 1)
    stat_s[t] = jnp.where(
        lane == 0,
        jnp.sum(final, axis=1, keepdims=True),
        jnp.sum(final * final, axis=1, keepdims=True),
    )
    send(stat_s.at[t], stat_s.at[t], small_sems, 2, partner)
    receive(stat_s.at[other], small_sems, 2)
    stats = (stat_s[0] + stat_s[1]) / model
    average, second = stats[:, 0:1], stats[:, 1:2]
    scaled = (final - average) * lax.rsqrt(second - average * average + epsilon)
    out[...] = (scaled * out_gain[t]).astype(jnp.bfloat16)
    for copy in pending:
        copy.wait_send()


def by_kernel(
    width,
    tokens,
    lin_weight,
    glu_weight,
    conv_taps,
    conv_gain,
    conv_out_weight,
    mix_gain,
    ff_gate,
    ff_up,
    ff_down,
    out_gain,
):
    n_fs, n_tp = lax.axis_size("fs"), lax.axis_size("tp")
    _, length, feat = tokens.shape
    rows, model = n_fs * length, feat * n_tp
    depth, own_chans = lin_weight.shape
    chans = own_chans // n_fs
    n_taps = conv_taps.shape[0]
    glu_mix = jnp.concatenate(
        (
            lin_weight.reshape(depth, n_fs, chans).transpose(1, 0, 2),
            glu_weight.reshape(depth, n_fs, chans).transpose(1, 0, 2),
        ),
        axis=2,
    )
    own_taps = lax.dynamic_slice_in_dim(conv_taps, lax.axis_index("fs") * chans, chans, 1)
    taps = jnp.concatenate((own_taps, own_taps), axis=1)
    vmem, far = pl.BlockSpec(memory_space=pltpu.VMEM), pl.BlockSpec(memory_space=pl.ANY)
    bf, fl = jnp.bfloat16, jnp.float32
    span = ff_down.shape[1]
    pair = lambda n: pltpu.SemaphoreType.DMA((2, n))
    result = pl.pallas_call(
        functools.partial(fused, n_fs, n_tp, width),
        out_shape=jax.ShapeDtypeStruct((length, feat), bf),
        in_specs=[vmem] * 6 + [far] * 3 + [vmem],
        out_specs=vmem,
        scratch_shapes=[
            pltpu.VMEM((n_tp, rows, feat), bf),
            pltpu.VMEM((n_fs * depth, 2 * chans), bf),
            pltpu.VMEM((n_tp, 1, own_chans), fl),
            pltpu.VMEM((n_tp, own_chans, span // n_tp), bf),
            pltpu.VMEM((n_fs // 2, length + 32, LANES), fl),
            pltpu.VMEM((n_fs * n_tp, rows // 2, LANES), bf),
            pltpu.VMEM((rows, own_chans * n_tp), fl),
            pltpu.VMEM((rows, own_chans * n_tp), bf),
            pltpu.VMEM((n_fs * n_tp, rows, LANES), bf),
            pltpu.VMEM((rows, model), bf),
            pltpu.VMEM((n_fs * depth, width), bf),
            pltpu.VMEM((n_fs * depth, width), bf),
            pltpu.VMEM((n_fs, width, span), bf),
            pltpu.VMEM((rows, width), bf),
            pltpu.VMEM((n_tp, rows, feat), bf),
            pltpu.VMEM((rows, feat), bf),
            pltpu.VMEM((rows, feat), bf),
            pltpu.VMEM((n_fs, length, feat), bf),
            pltpu.VMEM((n_tp, length, LANES), fl),
            pair(n_fs),
            pair(3),
            pair(2 * n_fs),
            pair(2 * n_fs),
            pair(2 * n_fs),
            pair(3 * n_fs),
            pair(3 * n_fs),
            pltpu.SemaphoreType.DMA((6,)),
            pair(n_fs),
            pair(n_fs),
        ],
        compiler_params=pltpu.CompilerParams(
            collective_id=0, has_side_effects=True, vmem_limit_bytes=60 * 2**20
        ),
    )(
        tokens[0],
        glu_mix,
        taps,
        conv_gain[None],
        conv_out_weight,
        mix_gain[None],
        ff_gate,
        ff_up,
        ff_down,
        out_gain.reshape(n_tp, 1, feat),
    )
    return result[None]


def on_device(*args):
    tokens, lin_weight, conv_out_weight, ff_gate = args[0], args[1], args[5], args[7]
    n_fs, n_tp, n_rep = (lax.axis_size(a) for a in ("fs", "tp", "rep"))
    seqs, length, feat = tokens.shape
    units = ff_gate.shape[1]
    width = -(-units // (n_fs * LANES)) * LANES
    fits = (
        n_rep == 2
        and n_tp == 2
        and n_fs % 4 == 0
        and seqs == 1
        and length % 16 == 0
        and args[3].shape[0] <= 33
        and lin_weight.shape[1] * 2 == n_fs * LANES
        and conv_out_weight.shape[1] == n_tp * LANES
        and feat % LANES == 0
        and units % LANES == 0
        and width * (n_fs - 1) < units
        and lin_weight.shape[0] % 32 == 0
    )
    if fits:
        return by_kernel(width, *args)
    return by_collectives(*args)


def solution(mesh):
    mapped = jax.shard_map(
        on_device,
        mesh=mesh,
        in_specs=(
            P(("rep", "fs"), None, "tp"),
            P("fs", "tp"),
            P("fs", "tp"),
            P(None, "tp"),
            P("tp"),
            P("tp", "fs"),
            P(),
            P("fs", "tp"),
            P("fs", "tp"),
            P("tp", "fs"),
            P(),
        ),
        out_specs=P(("rep", "fs"), None, "tp"),
        check_vma=False,
    )
    return mapped
```

```python
import functools

import jax
import jax.numpy as jnp
from jax import lax
from jax.experimental import pallas as pl
from jax.experimental.pallas import tpu as pltpu
from jax.sharding import PartitionSpec as P

residual_scale = 2.0**0.25
epsilon = 1e-05


def normed(values):
    average = jnp.mean(values, axis=-1, keepdims=True)
    second = jnp.mean(values * values, axis=-1, keepdims=True)
    return (values - average) * lax.rsqrt(second - average * average + epsilon)


def interleave(left, right, parts):
    rows, width = left.shape
    pair = jnp.concatenate(
        (left.reshape(rows, parts, width // parts), right.reshape(rows, parts, width // parts)),
        axis=2,
    )
    return pair.reshape(rows, 2 * width)


def by_collectives(
    tokens,
    lin_weight,
    glu_weight,
    conv_taps,
    conv_gain,
    conv_out_weight,
    mix_gain,
    ff_gate,
    ff_up,
    ff_down,
    out_gain,
):
    n_fs, n_tp = lax.axis_size("fs"), lax.axis_size("tp")
    fs_index, tp_index = lax.axis_index("fs"), lax.axis_index("tp")
    seqs, length, feat = tokens.shape
    groups = n_fs * seqs
    rows = groups * length
    model = feat * n_tp
    conv_gain_all = lax.all_gather(conv_gain, "tp", axis=0, tiled=True)

    gathered = lax.all_gather(tokens, ("fs", "tp"), axis=0, tiled=False)
    all_tokens = (
        gathered.reshape(n_fs, n_tp, seqs, length, feat)
        .transpose(0, 2, 3, 1, 4)
        .reshape(rows, model)
    )
    glu_pair = lax.all_to_all(
        interleave(lin_weight, glu_weight, n_fs), "fs", split_axis=1, concat_axis=0, tiled=True
    )
    own_out = lax.all_to_all(conv_out_weight, "tp", split_axis=1, concat_axis=0, tiled=True)
    ff_pair = lax.all_to_all(
        interleave(ff_gate, ff_up, n_fs), "fs", split_axis=1, concat_axis=0, tiled=True
    )
    own_down = lax.all_to_all(ff_down, "fs", split_axis=0, concat_axis=1, tiled=True)

    chans = glu_pair.shape[1] // 2
    product = jnp.dot(all_tokens, glu_pair, preferred_element_type=jnp.float32)
    glu = (product[:, :chans] * jax.nn.sigmoid(product[:, chans:])).astype(jnp.bfloat16)
    n_taps = conv_taps.shape[0]
    margin = (n_taps - 1) // 2
    own_taps = lax.dynamic_slice_in_dim(conv_taps, fs_index * chans, chans, 1)
    padded = jnp.pad(
        glu.astype(jnp.float32).reshape(groups, length, chans),
        ((0, 0), (margin, margin), (0, 0)),
    )
    conv = sum(padded[:, k : k + length] * own_taps[k] for k in range(n_taps))
    conv = conv.reshape(rows, chans).astype(jnp.bfloat16)
    conv_all = lax.all_gather(conv, ("tp", "fs"), axis=1, tiled=True)
    activated = jax.nn.silu(normed(conv_all.astype(jnp.float32)) * conv_gain_all).astype(
        jnp.bfloat16
    )
    mixed_own = jnp.dot(activated, own_out, preferred_element_type=jnp.float32).astype(
        jnp.bfloat16
    )
    mixed = lax.all_gather(mixed_own, ("fs", "tp"), axis=1, tiled=True)
    before = residual_scale * all_tokens.astype(jnp.float32) + mixed.astype(jnp.float32)
    middle = (normed(before) * mix_gain).astype(jnp.bfloat16)

    units = ff_pair.shape[1] // 2
    both = jnp.dot(middle, ff_pair, preferred_element_type=jnp.float32)
    hidden = (jax.nn.silu(both[:, :units]) * both[:, units:]).astype(jnp.bfloat16)
    down = jnp.dot(hidden, own_down, preferred_element_type=jnp.float32).astype(jnp.bfloat16)
    sends = (
        down.reshape(n_fs, seqs * length, n_tp, feat)
        .transpose(0, 2, 1, 3)
        .reshape(n_fs * n_tp, seqs * length, feat)
    )
    arrived = lax.all_to_all(sends, ("fs", "tp"), split_axis=0, concat_axis=0, tiled=True)
    forward = jnp.sum(arrived.astype(jnp.float32), axis=0)
    forward = forward.astype(jnp.bfloat16).astype(jnp.float32)
    middle_own = lax.dynamic_slice(
        middle,
        (fs_index * seqs * length, tp_index * feat),
        (seqs * length, feat),
    )
    final = residual_scale * middle_own.astype(jnp.float32) + forward
    sums, squares = lax.psum(
        (jnp.sum(final, axis=1, keepdims=True), jnp.sum(final * final, axis=1, keepdims=True)),
        "tp",
    )
    average = sums / model
    out = (final - average) * lax.rsqrt(squares / model - average * average + epsilon)
    gain = lax.dynamic_slice_in_dim(out_gain, tp_index * feat, feat, 0)
    return (out * gain).astype(jnp.bfloat16).reshape(seqs, length, feat)


MESH = pl.DeviceIdType.MESH
LANES = 128


def fused(
    n_fs,
    n_tp,
    width,
    tok,
    glu_mix,
    taps,
    gain,
    out_weight,
    mix_gain,
    gate_hbm,
    up_hbm,
    down_hbm,
    out_gain,
    out,
    x_s,
    glu_s,
    gain_s,
    proj_s,
    pad_s,
    conv_s,
    norm_s,
    act_s,
    mixed_s,
    mid_s,
    gate_s,
    up_s,
    down_s,
    hid_s,
    part_s,
    half_s,
    sum_s,
    q_s,
    stat_s,
    glu_sems,
    small_sems,
    tok_sems,
    conv_sems,
    mixed_sems,
    ff_sems,
    cross_sems,
    local_sems,
    half_sems,
    q_sems,
    y_s,
    y_sems,
    glu_cross_sems,
):
    rep, f, t = lax.axis_index("rep"), lax.axis_index("fs"), lax.axis_index("tp")
    other = 1 - t
    n_hi = n_fs // 2
    hi, lo = f // 2, f % 2
    rows, feat = x_s.shape[1:]
    length = rows // n_fs
    model = feat * n_tp
    depth = gate_hbm.shape[0]
    half_depth = depth // 2
    total = gate_hbm.shape[1]
    chans = LANES // 2
    pending = []

    barrier = pltpu.get_barrier_semaphore()
    for d in range(n_fs):
        for e in range(n_tp):
            if d or e:
                pl.semaphore_signal(
                    barrier,
                    inc=1,
                    device_id=(rep, (f + d) % n_fs, (t + e) % n_tp),
                    device_id_type=MESH,
                )
    pl.semaphore_signal(barrier, inc=1, device_id=(1 - rep, f, t), device_id_type=MESH)
    pl.semaphore_wait(barrier, n_fs * n_tp)

    def remote(src, dst, sems, index, device):
        return pltpu.make_async_remote_copy(
            src_ref=src,
            dst_ref=dst,
            send_sem=sems.at[0, index],
            recv_sem=sems.at[1, index],
            device_id=device,
            device_id_type=MESH,
        )

    def send(*parts):
        copy = remote(*parts)
        copy.start()
        pending.append(copy)

    partner = (rep, f, other)

    def receive(dst, sems, index):
        remote(dst, dst, sems, index, partner).wait_recv()

    def at(step, low):
        return ((hi - step + n_hi) % n_hi) * 2 + low

    def gather_start(own, slot, sems):
        for d in range(1, n_hi):
            send(own, slot(f, t), sems, d, (rep, ((hi + d) % n_hi) * 2 + lo, t))
        send(own, slot(f, t), sems, n_hi, (rep, hi * 2 + 1 - lo, t))
        send(own, slot(f, t), sems, 2 * n_hi, partner)

    def gather_finish(slot, sems):
        for d in range(1, n_hi):
            block = slot(at(d, lo), t)
            receive(block, sems, d)
            send(block, block, sems, n_hi + d, (rep, hi * 2 + 1 - lo, t))
            send(block, block, sems, 2 * n_hi + d, partner)
        for d in range(n_hi):
            block = slot(at(d, 1 - lo), t)
            receive(block, sems, n_hi + d)
            send(block, block, sems, 3 * n_hi + d, partner)
        for d in range(n_hi):
            receive(slot(at(d, lo), other), sems, 2 * n_hi + d)
            receive(slot(at(d, 1 - lo), other), sems, 3 * n_hi + d)

    def tok_slot(i, j):
        return x_s.at[j, pl.ds(pl.multiple_of(i * length, length), length)]

    def half_rows(i, part):
        return pl.ds(pl.multiple_of(i * depth + part * half_depth, half_depth), half_depth)

    gather_start(tok, tok_slot, tok_sems)
    for d in range(1, n_fs):
        to = (f + d) % n_fs
        send(
            glu_mix.at[to, half_rows(0, rep)],
            glu_s.at[half_rows(f, rep)],
            glu_sems,
            d,
            (rep, to, t),
        )
    send(gain, gain_s.at[t], small_sems, 0, partner)
    columns = pl.ds(pl.multiple_of(other * LANES, LANES), LANES)
    own_columns = pl.ds(pl.multiple_of(t * LANES, LANES), LANES)
    send(out_weight.at[:, columns], proj_s.at[t], small_sems, 1, partner)

    def start_of(i):
        return pl.multiple_of(i * width - (i // (n_fs - 1)) * (n_fs * width - total), LANES)

    half_width = width // 2

    def pieces(to, source, part):
        first = start_of(to)
        ups = pl.ds(pl.multiple_of(part * half_depth, half_depth), half_depth)
        spot = pl.ds(pl.multiple_of(source * depth + part * half_depth, half_depth), half_depth)
        deep = pl.ds(pl.multiple_of(part * half_width, half_width), half_width)
        from_down = pl.ds(pl.multiple_of(first + part * half_width, LANES // 2), half_width)
        return (
            (gate_hbm.at[ups, pl.ds(first, width)], gate_s.at[spot]),
            (up_hbm.at[ups, pl.ds(first, width)], up_s.at[spot]),
            (down_hbm.at[from_down], down_s.at[source, deep]),
        )

    order = range(1, n_fs)
    early, late = range(1, n_fs // 2 + 1), range(n_fs // 2 + 1, n_fs)

    def weights_start(which, order=order):
        for d in order:
            to = (f + d) % n_fs
            src, dst = pieces(to, f, rep)[which]
            send(src, dst, ff_sems, which * n_fs + d, (rep, to, t))

    def weights_forward(which, order=order):
        for d in order:
            dst = pieces(f, (f - d + n_fs) % n_fs, rep)[which][1]
            receive(dst, ff_sems, which * n_fs + d)
            send(dst, dst, cross_sems, which * n_fs + d, (1 - rep, f, t))

    def weights_finish(which):
        for d in order:
            dst = pieces(f, (f - d + n_fs) % n_fs, 1 - rep)[which][1]
            receive(dst, cross_sems, which * n_fs + d)

    weights_start(0)
    weights_start(1)
    own_copies = []
    for which in range(3):
        for part in range(2):
            src, dst = pieces(f, f, part)[which]
            own_copies.append(
                pltpu.make_async_copy(src, dst, local_sems.at[which * 2 + part])
            )
    for copy in own_copies:
        copy.start()

    x_s[t, pl.ds(pl.multiple_of(f * length, length), length), :] = tok[...]
    glu_s[pl.ds(pl.multiple_of(f * depth, depth), depth), :] = glu_mix[f]
    gain_s[t] = gain[...]
    proj_s[t] = out_weight[:, own_columns]
    pad_s[...] = jnp.zeros_like(pad_s)

    gather_finish(tok_slot, tok_sems)
    for d in range(1, n_fs):
        block = glu_s.at[half_rows((f - d + n_fs) % n_fs, rep)]
        receive(block, glu_sems, d)
        send(block, block, glu_cross_sems, d, (1 - rep, f, t))
    for d in range(1, n_fs):
        block = glu_s.at[half_rows((f - d + n_fs) % n_fs, 1 - rep)]
        receive(block, glu_cross_sems, d)

    product = sum(
        jnp.dot(
            x_s[j], glu_s[j * feat : (j + 1) * feat], preferred_element_type=jnp.float32
        )
        for j in range(n_tp)
    )
    glu = product[:, :chans] / (1.0 + jnp.exp(-product[:, chans:]))
    top = rows // 2
    packed = jnp.concatenate((glu[:top], glu[top:]), axis=1)
    packed = packed.astype(jnp.bfloat16).astype(jnp.float32)
    n_taps = taps.shape[0]
    margin = (n_taps - 1) // 2
    conv_slot = lambda i, j: conv_s.at[j * n_fs + i]
    groups = n_fs // 2
    for g in range(groups):
        pad_s[g, 16 : 16 + length, :] = packed[g * length : (g + 1) * length]
    for g in range(groups):
        acc = jnp.zeros((length, LANES), jnp.float32)
        for k in range(n_taps):
            first = 16 - margin + k
            acc = acc + pad_s[g, first : first + length, :] * taps[k : k + 1, :]
        conv_s[t * n_fs + f, g * length : (g + 1) * length, :] = acc.astype(jnp.bfloat16)
    gather_start(conv_slot(f, t), conv_slot, conv_sems)
    weights_start(2, early)
    weights_forward(0)
    weights_forward(1)
    gather_finish(conv_slot, conv_sems)
    receive(gain_s.at[other], small_sems, 0)
    receive(proj_s.at[other], small_sems, 1)

    for j in range(n_fs * n_tp // 2):
        left = conv_s[2 * j].astype(jnp.float32)
        right = conv_s[2 * j + 1].astype(jnp.float32)
        cols = slice(j * LANES, (j + 1) * LANES)
        norm_s[:top, cols] = jnp.concatenate((left[:, :chans], right[:, :chans]), axis=1)
        norm_s[top:, cols] = jnp.concatenate((left[:, chans:], right[:, chans:]), axis=1)
    gains = jnp.concatenate([gain_s[j] for j in range(n_tp)], axis=1)

    @pl.loop(0, n_fs)
    def _(i):
        here = pl.ds(pl.multiple_of(i * length, length), length)
        v = normed(norm_s[here, :]) * gains
        act_s[here, :] = (v / (1.0 + jnp.exp(-v))).astype(jnp.bfloat16)

    share = proj_s.shape[1]
    mixed_slot = lambda i, j: mixed_s.at[i * n_tp + j]
    mixed_s[f * n_tp + t] = sum(
        jnp.dot(
            act_s[:, j * share : (j + 1) * share],
            proj_s[j],
            preferred_element_type=jnp.float32,
        )
        for j in range(n_tp)
    ).astype(jnp.bfloat16)
    gather_start(mixed_slot(f, t), mixed_slot, mixed_sems)
    weights_start(2, late)
    weights_forward(2, early)
    gather_finish(mixed_slot, mixed_sems)

    @pl.loop(0, n_fs)
    def _(i):
        here = pl.ds(pl.multiple_of(i * length, length), length)
        skip = jnp.concatenate([x_s[j, here, :] for j in range(n_tp)], axis=1)
        added = jnp.concatenate([mixed_s[j, here, :] for j in range(n_fs * n_tp)], axis=1)
        before = residual_scale * skip.astype(jnp.float32) + added.astype(jnp.float32)
        mid_s[here, :] = (normed(before) * mix_gain[...]).astype(jnp.bfloat16)

    for copy in own_copies:
        copy.wait()
    weights_finish(0)
    weights_finish(1)
    keep = lax.broadcasted_iota(jnp.int32, (1, width), 1) + start_of(f) >= f * width

    for i in range(2):
        here = pl.ds(i * top, top)
        gate = jnp.dot(mid_s[here, :], gate_s[...], preferred_element_type=jnp.float32)
        upward = jnp.dot(mid_s[here, :], up_s[...], preferred_element_type=jnp.float32)
        value = gate / (1.0 + jnp.exp(-gate)) * upward
        hid_s[here, :] = jnp.where(keep, value, 0.0).astype(jnp.bfloat16)
        if i == 0:
            weights_forward(2, late)

    weights_finish(2)
    span = down_s.shape[2]
    per_half = n_fs // n_tp

    def project(side):
        @pl.loop(0, per_half)
        def _(j):
            part_s[side, :, pl.ds(pl.multiple_of(j * span, span), span)] = jnp.dot(
                hid_s[...], down_s[side * per_half + j], preferred_element_type=jnp.float32
            ).astype(jnp.bfloat16)

    def rows_of(i):
        return pl.ds(pl.multiple_of(i * length, length), length)

    def toward(step, low):
        return ((hi + step) % n_hi) * 2 + low

    steps = list(range(1, n_hi)) + [0]
    project(other)
    for d in steps:
        for e, low in enumerate((1 - lo, lo)):
            here = rows_of(toward(d, low))
            send(part_s.at[other, here], half_s.at[here], half_sems, 2 * d + e, partner)
    project(t)
    for d in steps:
        here = rows_of(toward(d, 1 - lo))
        receive(half_s.at[here], half_sems, 2 * d)
        both = part_s[t, here, :].astype(jnp.float32) + half_s[here, :].astype(jnp.float32)
        sum_s[here, :] = both.astype(jnp.bfloat16)
        send(sum_s.at[here], y_s.at[d], y_sems, d, (rep, hi * 2 + 1 - lo, t))
    for d in steps:
        to = toward(d, lo)
        here = rows_of(to)
        receive(half_s.at[here], half_sems, 2 * d + 1)
        both = part_s[t, here, :].astype(jnp.float32) + half_s[here, :].astype(jnp.float32)
        receive(y_s.at[d], y_sems, d)
        forward = both + y_s[d].astype(jnp.float32)
        if d:
            sum_s[here, :] = forward.astype(jnp.bfloat16)
            send(sum_s.at[here], q_s.at[d], q_sems, d, (rep, to, t))
    for d in range(1, n_hi):
        receive(q_s.at[d], q_sems, d)
        forward = forward + q_s[d].astype(jnp.float32)
    forward = forward.astype(jnp.bfloat16).astype(jnp.float32)
    own_half = pl.ds(pl.multiple_of(t * feat, feat), feat)
    final = residual_scale * mid_s[rows_of(f), own_half].astype(jnp.float32) + forward
    lane = lax.broadcasted_iota(jnp.int32, (length, LANES), 1)
    stat_s[t] = jnp.where(
        lane == 0,
        jnp.sum(final, axis=1, keepdims=True),
        jnp.sum(final * final, axis=1, keepdims=True),
    )
    send(stat_s.at[t], stat_s.at[t], small_sems, 2, partner)
    receive(stat_s.at[other], small_sems, 2)
    stats = (stat_s[0] + stat_s[1]) / model
    average, second = stats[:, 0:1], stats[:, 1:2]
    scaled = (final - average) * lax.rsqrt(second - average * average + epsilon)
    out[...] = (scaled * out_gain[t]).astype(jnp.bfloat16)
    for copy in pending:
        copy.wait_send()


def by_kernel(
    width,
    tokens,
    lin_weight,
    glu_weight,
    conv_taps,
    conv_gain,
    conv_out_weight,
    mix_gain,
    ff_gate,
    ff_up,
    ff_down,
    out_gain,
):
    n_fs, n_tp = lax.axis_size("fs"), lax.axis_size("tp")
    _, length, feat = tokens.shape
    rows, model = n_fs * length, feat * n_tp
    depth, own_chans = lin_weight.shape
    chans = own_chans // n_fs
    n_taps = conv_taps.shape[0]
    glu_mix = jnp.concatenate(
        (
            lin_weight.reshape(depth, n_fs, chans).transpose(1, 0, 2),
            glu_weight.reshape(depth, n_fs, chans).transpose(1, 0, 2),
        ),
        axis=2,
    )
    own_taps = lax.dynamic_slice_in_dim(conv_taps, lax.axis_index("fs") * chans, chans, 1)
    taps = jnp.concatenate((own_taps, own_taps), axis=1)
    vmem, far = pl.BlockSpec(memory_space=pltpu.VMEM), pl.BlockSpec(memory_space=pl.ANY)
    bf, fl = jnp.bfloat16, jnp.float32
    span = ff_down.shape[1]
    pair = lambda n: pltpu.SemaphoreType.DMA((2, n))
    result = pl.pallas_call(
        functools.partial(fused, n_fs, n_tp, width),
        out_shape=jax.ShapeDtypeStruct((length, feat), bf),
        in_specs=[vmem] * 6 + [far] * 3 + [vmem],
        out_specs=vmem,
        scratch_shapes=[
            pltpu.VMEM((n_tp, rows, feat), bf),
            pltpu.VMEM((n_fs * depth, 2 * chans), bf),
            pltpu.VMEM((n_tp, 1, own_chans), fl),
            pltpu.VMEM((n_tp, own_chans, span // n_tp), bf),
            pltpu.VMEM((n_fs // 2, length + 32, LANES), fl),
            pltpu.VMEM((n_fs * n_tp, rows // 2, LANES), bf),
            pltpu.VMEM((rows, own_chans * n_tp), fl),
            pltpu.VMEM((rows, own_chans * n_tp), bf),
            pltpu.VMEM((n_fs * n_tp, rows, LANES), bf),
            pltpu.VMEM((rows, model), bf),
            pltpu.VMEM((n_fs * depth, width), bf),
            pltpu.VMEM((n_fs * depth, width), bf),
            pltpu.VMEM((n_fs, width, span), bf),
            pltpu.VMEM((rows, width), bf),
            pltpu.VMEM((n_tp, rows, feat), bf),
            pltpu.VMEM((rows, feat), bf),
            pltpu.VMEM((rows, feat), bf),
            pltpu.VMEM((n_fs // 2, length, feat), bf),
            pltpu.VMEM((n_tp, length, LANES), fl),
            pair(n_fs),
            pair(3),
            pair(2 * n_fs),
            pair(2 * n_fs),
            pair(2 * n_fs),
            pair(3 * n_fs),
            pair(3 * n_fs),
            pltpu.SemaphoreType.DMA((6,)),
            pair(n_fs),
            pair(n_fs // 2),
            pltpu.VMEM((n_fs // 2, length, feat), bf),
            pair(n_fs // 2),
            pair(n_fs),
        ],
        compiler_params=pltpu.CompilerParams(
            collective_id=0, has_side_effects=True, vmem_limit_bytes=60 * 2**20
        ),
    )(
        tokens[0],
        glu_mix,
        taps,
        conv_gain[None],
        conv_out_weight,
        mix_gain[None],
        ff_gate,
        ff_up,
        ff_down,
        out_gain.reshape(n_tp, 1, feat),
    )
    return result[None]


def on_device(*args):
    tokens, lin_weight, conv_out_weight, ff_gate = args[0], args[1], args[5], args[7]
    n_fs, n_tp, n_rep = (lax.axis_size(a) for a in ("fs", "tp", "rep"))
    seqs, length, feat = tokens.shape
    units = ff_gate.shape[1]
    width = -(-units // (n_fs * LANES)) * LANES
    fits = (
        n_rep == 2
        and n_tp == 2
        and n_fs % 4 == 0
        and seqs == 1
        and length % 16 == 0
        and args[3].shape[0] <= 33
        and lin_weight.shape[1] * 2 == n_fs * LANES
        and conv_out_weight.shape[1] == n_tp * LANES
        and feat % LANES == 0
        and units % LANES == 0
        and width * (n_fs - 1) < units
        and lin_weight.shape[0] % 32 == 0
    )
    if fits:
        return by_kernel(width, *args)
    return by_collectives(*args)


def solution(mesh):
    mapped = jax.shard_map(
        on_device,
        mesh=mesh,
        in_specs=(
            P(("rep", "fs"), None, "tp"),
            P("fs", "tp"),
            P("fs", "tp"),
            P(None, "tp"),
            P("tp"),
            P("tp", "fs"),
            P(),
            P("fs", "tp"),
            P("fs", "tp"),
            P("tp", "fs"),
            P(),
        ),
        out_specs=P(("rep", "fs"), None, "tp"),
        check_vma=False,
    )
    return mapped
```

```python
import functools

import jax
import jax.numpy as jnp
from jax import lax
from jax.experimental import pallas as pl
from jax.experimental.pallas import tpu as pltpu
from jax.sharding import PartitionSpec as P

residual_scale = 2.0**0.25
epsilon = 1e-05


def normed(values):
    average = jnp.mean(values, axis=-1, keepdims=True)
    second = jnp.mean(values * values, axis=-1, keepdims=True)
    return (values - average) * lax.rsqrt(second - average * average + epsilon)


def interleave(left, right, parts):
    rows, width = left.shape
    pair = jnp.concatenate(
        (left.reshape(rows, parts, width // parts), right.reshape(rows, parts, width // parts)),
        axis=2,
    )
    return pair.reshape(rows, 2 * width)


def by_collectives(
    tokens,
    lin_weight,
    glu_weight,
    conv_taps,
    conv_gain,
    conv_out_weight,
    mix_gain,
    ff_gate,
    ff_up,
    ff_down,
    out_gain,
):
    n_fs, n_tp = lax.axis_size("fs"), lax.axis_size("tp")
    fs_index, tp_index = lax.axis_index("fs"), lax.axis_index("tp")
    seqs, length, feat = tokens.shape
    groups = n_fs * seqs
    rows = groups * length
    model = feat * n_tp
    conv_gain_all = lax.all_gather(conv_gain, "tp", axis=0, tiled=True)

    gathered = lax.all_gather(tokens, ("fs", "tp"), axis=0, tiled=False)
    all_tokens = (
        gathered.reshape(n_fs, n_tp, seqs, length, feat)
        .transpose(0, 2, 3, 1, 4)
        .reshape(rows, model)
    )
    glu_pair = lax.all_to_all(
        interleave(lin_weight, glu_weight, n_fs), "fs", split_axis=1, concat_axis=0, tiled=True
    )
    own_out = lax.all_to_all(conv_out_weight, "tp", split_axis=1, concat_axis=0, tiled=True)
    ff_pair = lax.all_to_all(
        interleave(ff_gate, ff_up, n_fs), "fs", split_axis=1, concat_axis=0, tiled=True
    )
    own_down = lax.all_to_all(ff_down, "fs", split_axis=0, concat_axis=1, tiled=True)

    chans = glu_pair.shape[1] // 2
    product = jnp.dot(all_tokens, glu_pair, preferred_element_type=jnp.float32)
    glu = (product[:, :chans] * jax.nn.sigmoid(product[:, chans:])).astype(jnp.bfloat16)
    n_taps = conv_taps.shape[0]
    margin = (n_taps - 1) // 2
    own_taps = lax.dynamic_slice_in_dim(conv_taps, fs_index * chans, chans, 1)
    padded = jnp.pad(
        glu.astype(jnp.float32).reshape(groups, length, chans),
        ((0, 0), (margin, margin), (0, 0)),
    )
    conv = sum(padded[:, k : k + length] * own_taps[k] for k in range(n_taps))
    conv = conv.reshape(rows, chans).astype(jnp.bfloat16)
    conv_all = lax.all_gather(conv, ("tp", "fs"), axis=1, tiled=True)
    activated = jax.nn.silu(normed(conv_all.astype(jnp.float32)) * conv_gain_all).astype(
        jnp.bfloat16
    )
    mixed_own = jnp.dot(activated, own_out, preferred_element_type=jnp.float32).astype(
        jnp.bfloat16
    )
    mixed = lax.all_gather(mixed_own, ("fs", "tp"), axis=1, tiled=True)
    before = residual_scale * all_tokens.astype(jnp.float32) + mixed.astype(jnp.float32)
    middle = (normed(before) * mix_gain).astype(jnp.bfloat16)

    units = ff_pair.shape[1] // 2
    both = jnp.dot(middle, ff_pair, preferred_element_type=jnp.float32)
    hidden = (jax.nn.silu(both[:, :units]) * both[:, units:]).astype(jnp.bfloat16)
    down = jnp.dot(hidden, own_down, preferred_element_type=jnp.float32).astype(jnp.bfloat16)
    sends = (
        down.reshape(n_fs, seqs * length, n_tp, feat)
        .transpose(0, 2, 1, 3)
        .reshape(n_fs * n_tp, seqs * length, feat)
    )
    arrived = lax.all_to_all(sends, ("fs", "tp"), split_axis=0, concat_axis=0, tiled=True)
    forward = jnp.sum(arrived.astype(jnp.float32), axis=0)
    forward = forward.astype(jnp.bfloat16).astype(jnp.float32)
    middle_own = lax.dynamic_slice(
        middle,
        (fs_index * seqs * length, tp_index * feat),
        (seqs * length, feat),
    )
    final = residual_scale * middle_own.astype(jnp.float32) + forward
    sums, squares = lax.psum(
        (jnp.sum(final, axis=1, keepdims=True), jnp.sum(final * final, axis=1, keepdims=True)),
        "tp",
    )
    average = sums / model
    out = (final - average) * lax.rsqrt(squares / model - average * average + epsilon)
    gain = lax.dynamic_slice_in_dim(out_gain, tp_index * feat, feat, 0)
    return (out * gain).astype(jnp.bfloat16).reshape(seqs, length, feat)


MESH = pl.DeviceIdType.MESH
LANES = 128


def fused(
    n_fs,
    n_tp,
    width,
    tok,
    glu_mix,
    taps,
    gain,
    out_weight,
    mix_gain,
    gate_hbm,
    up_hbm,
    down_hbm,
    out_gain,
    out,
    x_s,
    glu_s,
    gain_s,
    proj_s,
    pad_s,
    conv_s,
    norm_s,
    act_s,
    mixed_s,
    mid_s,
    gate_s,
    up_s,
    down_s,
    hid_s,
    part_s,
    half_s,
    sum_s,
    q_s,
    stat_s,
    glu_sems,
    small_sems,
    tok_sems,
    conv_sems,
    mixed_sems,
    ff_sems,
    cross_sems,
    local_sems,
    half_sems,
    q_sems,
    y_s,
    y_sems,
    glu_cross_sems,
):
    rep, f, t = lax.axis_index("rep"), lax.axis_index("fs"), lax.axis_index("tp")
    other = 1 - t
    n_hi = n_fs // 2
    hi, lo = f // 2, f % 2
    rows, feat = x_s.shape[1:]
    length = rows // n_fs
    model = feat * n_tp
    depth = gate_hbm.shape[0]
    half_depth = depth // 2
    total = gate_hbm.shape[1]
    chans = LANES // 2
    pending = []

    barrier = pltpu.get_barrier_semaphore()
    for d in range(n_fs):
        for e in range(n_tp):
            if d or e:
                pl.semaphore_signal(
                    barrier,
                    inc=1,
                    device_id=(rep, (f + d) % n_fs, (t + e) % n_tp),
                    device_id_type=MESH,
                )
    pl.semaphore_signal(barrier, inc=1, device_id=(1 - rep, f, t), device_id_type=MESH)
    pl.semaphore_wait(barrier, n_fs * n_tp)

    def remote(src, dst, sems, index, device):
        return pltpu.make_async_remote_copy(
            src_ref=src,
            dst_ref=dst,
            send_sem=sems.at[0, index],
            recv_sem=sems.at[1, index],
            device_id=device,
            device_id_type=MESH,
        )

    def send(*parts):
        copy = remote(*parts)
        copy.start()
        pending.append(copy)

    partner = (rep, f, other)

    def receive(dst, sems, index):
        remote(dst, dst, sems, index, partner).wait_recv()

    def at(step, low):
        return ((hi - step + n_hi) % n_hi) * 2 + low

    def gather_start(own, slot, sems):
        for d in range(1, n_hi):
            send(own, slot(f, t), sems, d, (rep, ((hi + d) % n_hi) * 2 + lo, t))
        send(own, slot(f, t), sems, n_hi, (rep, hi * 2 + 1 - lo, t))
        send(own, slot(f, t), sems, 2 * n_hi, partner)

    def gather_finish(slot, sems):
        for d in range(1, n_hi):
            block = slot(at(d, lo), t)
            receive(block, sems, d)
            send(block, block, sems, n_hi + d, (rep, hi * 2 + 1 - lo, t))
            send(block, block, sems, 2 * n_hi + d, partner)
        for d in range(n_hi):
            block = slot(at(d, 1 - lo), t)
            receive(block, sems, n_hi + d)
            send(block, block, sems, 3 * n_hi + d, partner)
        for d in range(n_hi):
            receive(slot(at(d, lo), other), sems, 2 * n_hi + d)
            receive(slot(at(d, 1 - lo), other), sems, 3 * n_hi + d)

    def tok_slot(i, j):
        return x_s.at[j, pl.ds(pl.multiple_of(i * length, length), length)]

    def half_rows(i, part):
        return pl.ds(pl.multiple_of(i * depth + part * half_depth, half_depth), half_depth)

    gather_start(tok, tok_slot, tok_sems)
    for d in range(1, n_fs):
        to = (f + d) % n_fs
        send(
            glu_mix.at[to, half_rows(0, rep)],
            glu_s.at[half_rows(f, rep)],
            glu_sems,
            d,
            (rep, to, t),
        )
    send(gain, gain_s.at[t], small_sems, 0, partner)
    columns = pl.ds(pl.multiple_of(other * LANES, LANES), LANES)
    own_columns = pl.ds(pl.multiple_of(t * LANES, LANES), LANES)
    send(out_weight.at[:, columns], proj_s.at[t], small_sems, 1, partner)

    def start_of(i):
        return pl.multiple_of(i * width - (i // (n_fs - 1)) * (n_fs * width - total), LANES)

    half_width = width // 2

    def pieces(to, source, part):
        first = start_of(to)
        ups = pl.ds(pl.multiple_of(part * half_depth, half_depth), half_depth)
        spot = pl.ds(pl.multiple_of(source * depth + part * half_depth, half_depth), half_depth)
        deep = pl.ds(pl.multiple_of(part * half_width, half_width), half_width)
        from_down = pl.ds(pl.multiple_of(first + part * half_width, LANES // 2), half_width)
        return (
            (gate_hbm.at[ups, pl.ds(first, width)], gate_s.at[spot]),
            (up_hbm.at[ups, pl.ds(first, width)], up_s.at[spot]),
            (down_hbm.at[from_down], down_s.at[source, deep]),
        )

    order = range(1, n_fs)
    early, late = range(1, n_fs // 4 + 1), range(n_fs // 4 + 1, n_fs)
    near, rest = range(1, n_fs // 2 + 1), range(n_fs // 2 + 1, n_fs)

    def weights_start(which, order=order):
        for d in order:
            to = (f + d) % n_fs
            src, dst = pieces(to, f, rep)[which]
            send(src, dst, ff_sems, which * n_fs + d, (rep, to, t))

    def weights_forward(which, order=order):
        for d in order:
            dst = pieces(f, (f - d + n_fs) % n_fs, rep)[which][1]
            receive(dst, ff_sems, which * n_fs + d)
            send(dst, dst, cross_sems, which * n_fs + d, (1 - rep, f, t))

    def weights_finish(which):
        for d in order:
            dst = pieces(f, (f - d + n_fs) % n_fs, 1 - rep)[which][1]
            receive(dst, cross_sems, which * n_fs + d)

    weights_start(0)
    own_copies = []
    for which in range(3):
        for part in range(2):
            src, dst = pieces(f, f, part)[which]
            own_copies.append(
                pltpu.make_async_copy(src, dst, local_sems.at[which * 2 + part])
            )
    for copy in own_copies:
        copy.start()

    x_s[t, pl.ds(pl.multiple_of(f * length, length), length), :] = tok[...]
    glu_s[pl.ds(pl.multiple_of(f * depth, depth), depth), :] = glu_mix[f]
    gain_s[t] = gain[...]
    proj_s[t] = out_weight[:, own_columns]
    pad_s[...] = jnp.zeros_like(pad_s)

    gather_finish(tok_slot, tok_sems)
    for d in range(1, n_fs):
        block = glu_s.at[half_rows((f - d + n_fs) % n_fs, rep)]
        receive(block, glu_sems, d)
        send(block, block, glu_cross_sems, d, (1 - rep, f, t))
    for d in range(1, n_fs):
        block = glu_s.at[half_rows((f - d + n_fs) % n_fs, 1 - rep)]
        receive(block, glu_cross_sems, d)

    product = sum(
        jnp.dot(
            x_s[j], glu_s[j * feat : (j + 1) * feat], preferred_element_type=jnp.float32
        )
        for j in range(n_tp)
    )
    glu = product[:, :chans] / (1.0 + jnp.exp(-product[:, chans:]))
    top = rows // 2
    packed = jnp.concatenate((glu[:top], glu[top:]), axis=1)
    packed = packed.astype(jnp.bfloat16).astype(jnp.float32)
    n_taps = taps.shape[0]
    margin = (n_taps - 1) // 2
    conv_slot = lambda i, j: conv_s.at[j * n_fs + i]
    groups = n_fs // 2
    for g in range(groups):
        pad_s[g, 16 : 16 + length, :] = packed[g * length : (g + 1) * length]
    for g in range(groups):
        acc = jnp.zeros((length, LANES), jnp.float32)
        for k in range(n_taps):
            first = 16 - margin + k
            acc = acc + pad_s[g, first : first + length, :] * taps[k : k + 1, :]
        conv_s[t * n_fs + f, g * length : (g + 1) * length, :] = acc.astype(jnp.bfloat16)
    gather_start(conv_slot(f, t), conv_slot, conv_sems)
    weights_start(1)
    weights_start(2, early)
    weights_forward(0)
    gather_finish(conv_slot, conv_sems)
    receive(gain_s.at[other], small_sems, 0)
    receive(proj_s.at[other], small_sems, 1)

    for j in range(n_fs * n_tp // 2):
        left = conv_s[2 * j].astype(jnp.float32)
        right = conv_s[2 * j + 1].astype(jnp.float32)
        cols = slice(j * LANES, (j + 1) * LANES)
        norm_s[:top, cols] = jnp.concatenate((left[:, :chans], right[:, :chans]), axis=1)
        norm_s[top:, cols] = jnp.concatenate((left[:, chans:], right[:, chans:]), axis=1)
    gains = jnp.concatenate([gain_s[j] for j in range(n_tp)], axis=1)

    @pl.loop(0, n_fs)
    def _(i):
        here = pl.ds(pl.multiple_of(i * length, length), length)
        v = normed(norm_s[here, :]) * gains
        act_s[here, :] = (v / (1.0 + jnp.exp(-v))).astype(jnp.bfloat16)

    weights_forward(1, near)
    share = proj_s.shape[1]
    mixed_slot = lambda i, j: mixed_s.at[i * n_tp + j]
    mixed_s[f * n_tp + t] = sum(
        jnp.dot(
            act_s[:, j * share : (j + 1) * share],
            proj_s[j],
            preferred_element_type=jnp.float32,
        )
        for j in range(n_tp)
    ).astype(jnp.bfloat16)
    gather_start(mixed_slot(f, t), mixed_slot, mixed_sems)
    weights_start(2, late)
    weights_forward(1, rest)
    weights_forward(2, early)
    gather_finish(mixed_slot, mixed_sems)

    @pl.loop(0, n_fs)
    def _(i):
        here = pl.ds(pl.multiple_of(i * length, length), length)
        skip = jnp.concatenate([x_s[j, here, :] for j in range(n_tp)], axis=1)
        added = jnp.concatenate([mixed_s[j, here, :] for j in range(n_fs * n_tp)], axis=1)
        before = residual_scale * skip.astype(jnp.float32) + added.astype(jnp.float32)
        mid_s[here, :] = (normed(before) * mix_gain[...]).astype(jnp.bfloat16)

    for copy in own_copies:
        copy.wait()
    weights_finish(0)
    weights_finish(1)
    keep = lax.broadcasted_iota(jnp.int32, (1, width), 1) + start_of(f) >= f * width

    for i in range(2):
        here = pl.ds(i * top, top)
        gate = jnp.dot(mid_s[here, :], gate_s[...], preferred_element_type=jnp.float32)
        upward = jnp.dot(mid_s[here, :], up_s[...], preferred_element_type=jnp.float32)
        value = gate / (1.0 + jnp.exp(-gate)) * upward
        hid_s[here, :] = jnp.where(keep, value, 0.0).astype(jnp.bfloat16)
        if i == 0:
            weights_forward(2, late)

    weights_finish(2)
    span = down_s.shape[2]
    per_half = n_fs // n_tp

    def project(side):
        @pl.loop(0, per_half)
        def _(j):
            part_s[side, :, pl.ds(pl.multiple_of(j * span, span), span)] = jnp.dot(
                hid_s[...], down_s[side * per_half + j], preferred_element_type=jnp.float32
            ).astype(jnp.bfloat16)

    def rows_of(i):
        return pl.ds(pl.multiple_of(i * length, length), length)

    def toward(step, low):
        return ((hi + step) % n_hi) * 2 + low

    steps = list(range(1, n_hi)) + [0]
    project(other)
    for d in steps:
        for e, low in enumerate((1 - lo, lo)):
            here = rows_of(toward(d, low))
            send(part_s.at[other, here], half_s.at[here], half_sems, 2 * d + e, partner)
    project(t)
    for d in steps:
        here = rows_of(toward(d, 1 - lo))
        receive(half_s.at[here], half_sems, 2 * d)
        both = part_s[t, here, :].astype(jnp.float32) + half_s[here, :].astype(jnp.float32)
        sum_s[here, :] = both.astype(jnp.bfloat16)
        send(sum_s.at[here], y_s.at[d], y_sems, d, (rep, hi * 2 + 1 - lo, t))
    for d in steps:
        to = toward(d, lo)
        here = rows_of(to)
        receive(half_s.at[here], half_sems, 2 * d + 1)
        both = part_s[t, here, :].astype(jnp.float32) + half_s[here, :].astype(jnp.float32)
        receive(y_s.at[d], y_sems, d)
        forward = both + y_s[d].astype(jnp.float32)
        if d:
            sum_s[here, :] = forward.astype(jnp.bfloat16)
            send(sum_s.at[here], q_s.at[d], q_sems, d, (rep, to, t))
    for d in range(1, n_hi):
        receive(q_s.at[d], q_sems, d)
        forward = forward + q_s[d].astype(jnp.float32)
    forward = forward.astype(jnp.bfloat16).astype(jnp.float32)
    own_half = pl.ds(pl.multiple_of(t * feat, feat), feat)
    final = residual_scale * mid_s[rows_of(f), own_half].astype(jnp.float32) + forward
    lane = lax.broadcasted_iota(jnp.int32, (length, LANES), 1)
    stat_s[t] = jnp.where(
        lane == 0,
        jnp.sum(final, axis=1, keepdims=True),
        jnp.sum(final * final, axis=1, keepdims=True),
    )
    send(stat_s.at[t], stat_s.at[t], small_sems, 2, partner)
    receive(stat_s.at[other], small_sems, 2)
    stats = (stat_s[0] + stat_s[1]) / model
    average, second = stats[:, 0:1], stats[:, 1:2]
    scaled = (final - average) * lax.rsqrt(second - average * average + epsilon)
    out[...] = (scaled * out_gain[t]).astype(jnp.bfloat16)
    for copy in pending:
        copy.wait_send()


def by_kernel(
    width,
    tokens,
    lin_weight,
    glu_weight,
    conv_taps,
    conv_gain,
    conv_out_weight,
    mix_gain,
    ff_gate,
    ff_up,
    ff_down,
    out_gain,
):
    n_fs, n_tp = lax.axis_size("fs"), lax.axis_size("tp")
    _, length, feat = tokens.shape
    rows, model = n_fs * length, feat * n_tp
    depth, own_chans = lin_weight.shape
    chans = own_chans // n_fs
    n_taps = conv_taps.shape[0]
    glu_mix = jnp.concatenate(
        (
            lin_weight.reshape(depth, n_fs, chans).transpose(1, 0, 2),
            glu_weight.reshape(depth, n_fs, chans).transpose(1, 0, 2),
        ),
        axis=2,
    )
    own_taps = lax.dynamic_slice_in_dim(conv_taps, lax.axis_index("fs") * chans, chans, 1)
    taps = jnp.concatenate((own_taps, own_taps), axis=1)
    vmem, far = pl.BlockSpec(memory_space=pltpu.VMEM), pl.BlockSpec(memory_space=pl.ANY)
    bf, fl = jnp.bfloat16, jnp.float32
    span = ff_down.shape[1]
    pair = lambda n: pltpu.SemaphoreType.DMA((2, n))
    result = pl.pallas_call(
        functools.partial(fused, n_fs, n_tp, width),
        out_shape=jax.ShapeDtypeStruct((length, feat), bf),
        in_specs=[vmem] * 6 + [far] * 3 + [vmem],
        out_specs=vmem,
        scratch_shapes=[
            pltpu.VMEM((n_tp, rows, feat), bf),
            pltpu.VMEM((n_fs * depth, 2 * chans), bf),
            pltpu.VMEM((n_tp, 1, own_chans), fl),
            pltpu.VMEM((n_tp, own_chans, span // n_tp), bf),
            pltpu.VMEM((n_fs // 2, length + 32, LANES), fl),
            pltpu.VMEM((n_fs * n_tp, rows // 2, LANES), bf),
            pltpu.VMEM((rows, own_chans * n_tp), fl),
            pltpu.VMEM((rows, own_chans * n_tp), bf),
            pltpu.VMEM((n_fs * n_tp, rows, LANES), bf),
            pltpu.VMEM((rows, model), bf),
            pltpu.VMEM((n_fs * depth, width), bf),
            pltpu.VMEM((n_fs * depth, width), bf),
            pltpu.VMEM((n_fs, width, span), bf),
            pltpu.VMEM((rows, width), bf),
            pltpu.VMEM((n_tp, rows, feat), bf),
            pltpu.VMEM((rows, feat), bf),
            pltpu.VMEM((rows, feat), bf),
            pltpu.VMEM((n_fs // 2, length, feat), bf),
            pltpu.VMEM((n_tp, length, LANES), fl),
            pair(n_fs),
            pair(3),
            pair(2 * n_fs),
            pair(2 * n_fs),
            pair(2 * n_fs),
            pair(3 * n_fs),
            pair(3 * n_fs),
            pltpu.SemaphoreType.DMA((6,)),
            pair(n_fs),
            pair(n_fs // 2),
            pltpu.VMEM((n_fs // 2, length, feat), bf),
            pair(n_fs // 2),
            pair(n_fs),
        ],
        compiler_params=pltpu.CompilerParams(
            collective_id=0, has_side_effects=True, vmem_limit_bytes=60 * 2**20
        ),
    )(
        tokens[0],
        glu_mix,
        taps,
        conv_gain[None],
        conv_out_weight,
        mix_gain[None],
        ff_gate,
        ff_up,
        ff_down,
        out_gain.reshape(n_tp, 1, feat),
    )
    return result[None]


def on_device(*args):
    tokens, lin_weight, conv_out_weight, ff_gate = args[0], args[1], args[5], args[7]
    n_fs, n_tp, n_rep = (lax.axis_size(a) for a in ("fs", "tp", "rep"))
    seqs, length, feat = tokens.shape
    units = ff_gate.shape[1]
    width = -(-units // (n_fs * LANES)) * LANES
    fits = (
        n_rep == 2
        and n_tp == 2
        and n_fs % 4 == 0
        and seqs == 1
        and length % 16 == 0
        and args[3].shape[0] <= 33
        and lin_weight.shape[1] * 2 == n_fs * LANES
        and conv_out_weight.shape[1] == n_tp * LANES
        and feat % LANES == 0
        and units % LANES == 0
        and width * (n_fs - 1) < units
        and lin_weight.shape[0] % 32 == 0
    )
    if fits:
        return by_kernel(width, *args)
    return by_collectives(*args)


def solution(mesh):
    mapped = jax.shard_map(
        on_device,
        mesh=mesh,
        in_specs=(
            P(("rep", "fs"), None, "tp"),
            P("fs", "tp"),
            P("fs", "tp"),
            P(None, "tp"),
            P("tp"),
            P("tp", "fs"),
            P(),
            P("fs", "tp"),
            P("fs", "tp"),
            P("tp", "fs"),
            P(),
        ),
        out_specs=P(("rep", "fs"), None, "tp"),
        check_vma=False,
    )
    return mapped
```
